768 devices in a mesh: ep: 48 (over z, x), tp: 16 (over y, core).
Axes of the slice: x: 4, y: 8, z: 12, core: 2. Of those that a mesh axis runs over, the one named last changes fastest.
Arguments:
- tokens: bfloat16 [6144, 2048], P('ep'), may hold values from -6 to 6
- norm_gain: float32 [2048], replicated, may hold values from 0.1 to 1.9
- expert_ids: int32 [6144, 2], P('ep'), may hold values from 0 to 47, all different within a row; in each aligned block of 128 rows (0 to 127, 128 to 255, ...) at most 10 rows name the same one
- route_weights: float32 [6144, 2], P('ep'), may hold values from 0.2 to 1
- w_gate: bfloat16 [48, 2048, 4096], P('ep', None, 'tp'), may hold values from -0.125 to 0.125
- w_up: bfloat16 [48, 2048, 4096], P('ep', None, 'tp'), may hold values from -0.125 to 0.125
- w_down: bfloat16 [48, 4096, 2048], P('ep', 'tp'), may hold values from -0.09375 to 0.09375
Outputs:
- combined: bfloat16 [6144, 2048], P('ep', 'tp')
The draws below stay inside these ranges and needn't reach their ends.
Inputs may be any that keep to these rules, and one draw needn't show every extreme that they name: `expert_ids`: each row names two different experts; among the rows of one device no expert is named more than 10 times, and in every draw some expert is named exactly 10 times there.
All inputs are finite; a program needn't handle non-finite values.
Results may differ from the reference program's by a relative error of at most 0.019.
Values may be sent and summed in bfloat16 or wider, within the bound.
A program may use at most 32 MiB of HBM per device.

```python
import math
import jax
import jax.numpy as jnp
import numpy as np
from jax import lax

D = 2048
FF = 4096
TOK_DEV = 128
EXPERTS = 48
CAP = 10
TOKENS = 6144
N_EP = 48
N_TP = 16


def block_scale(own_key, extent, pieces, low, top_value):
    loudness = 1.0
    for axis_at, blocks in pieces:
        draws = jax.random.uniform(jax.random.fold_in(jax.random.fold_in(own_key, 6), axis_at), (blocks,), jnp.float32, low / len(pieces), top_value / len(pieces))
        loudness = loudness * jnp.repeat(jnp.exp(draws), extent[axis_at] // blocks).reshape((-1,) + (1,) * (len(extent) - 1 - axis_at))
    return loudness


def routed_block(own_key, own, number, rows, count, top, bound, lean):
    sequence = jax.random.permutation(own_key, count)
    heavy_load, ordinary = shares(count, rows * top, bound, lean, True), shares(count, rows * top, bound, lean, False)
    places = jnp.arange(count)

    def named(sizes, turn):
        used = int((sizes > 0).sum())
        fixed = max(1, used // 4)
        passed = fixed + (places - fixed + turn * (used - fixed)) % max(1, count - fixed)
        return jnp.zeros((count,), jnp.int32).at[sequence[jnp.where(places < fixed, places, passed)]].set(jnp.asarray(sizes, jnp.int32))

    sizes = jnp.where(number % 4 == 0, named(heavy_load, number // 4), named(ordinary, number - number // 4 - 1))
    mixed = jax.random.permutation(jax.random.fold_in(own, 3), count)
    giver, sink = mixed[0:count // 2 * 2:2], mixed[1:count // 2 * 2:2]
    margin = jnp.minimum(sizes[giver] - 1, bound - sizes[sink]) // 2
    margin = jnp.where((giver == sequence[0]) | (sink == sequence[0]) | (sizes[sink] == 0), 0, jnp.maximum(margin, 0))
    passed = jax.random.randint(jax.random.fold_in(own, 4), (count // 2,), 0, 1 << 20) % (margin + 1)
    sizes = sizes.at[giver].add(-passed).at[sink].add(passed)
    items = jnp.searchsorted(jnp.cumsum(sizes), jnp.arange(rows * top), side="right").astype(jnp.int32)
    listing = items.reshape(top, rows).T
    listing = listing[jax.random.permutation(jax.random.fold_in(own, 1), rows)]
    turn = jax.random.randint(jax.random.fold_in(own, 2), (rows, 1), 0, top)
    return jnp.take_along_axis(listing, (jnp.arange(top)[None, :] + turn) % top, axis=1)


def shares(count, total, reach, slope, full):
    portions = [(1 << 20) // math.isqrt(rank ** slope) + 1 for rank in range(1, count + 1)]
    largest = reach if full else min(reach, max(-(-total // count), total * portions[0] // sum(portions)))
    least = 1 if total - largest >= count - 1 else 0
    counts, spare = [largest] + [least] * (count - 1), total - largest - least * (count - 1)
    while spare > 0:
        candidates = [i for i in range(1, count) if counts[i] < largest] or [i for i in range(1, count) if counts[i] < reach]
        mass, budget = sum([portions[i] for i in candidates]), spare
        for i in candidates:
            more = min(reach - counts[i], max(1, budget * portions[i] // mass), spare)
            counts[i] = counts[i] + more
            spare = spare - more
    return np.array(counts)


def centred(stream_key, extent, width, limit, shards=(), kind=jnp.bfloat16):
    result = width * jax.random.normal(stream_key, extent, jnp.float32)
    if shards:
        result = result * block_scale(stream_key, extent, shards, -0.22, 0.18)
    return jnp.clip(result, -limit, limit).astype(kind)


def setup_inputs(seed: int = 0) -> dict:
    seeds = jax.random.split(jax.random.key(seed), 8)
    tokens = centred(seeds[0], (TOKENS, D), 1.0, 6.0, ((0, 48),))
    norm_gain = jnp.clip(1.0 + 0.18 * jax.random.normal(seeds[1], (D,), jnp.float32), 0.1, 1.9)
    expert_ids_keys = jax.random.split(jax.random.fold_in(seeds[2], 1), TOKENS // TOK_DEV)
    expert_ids_turns = jax.random.permutation(jax.random.fold_in(seeds[2], 3), TOKENS // TOK_DEV)
    expert_ids = jax.vmap(lambda own, number: routed_block(jax.random.fold_in(seeds[2], 2), own, number, TOK_DEV, EXPERTS, 2, CAP, 2))(expert_ids_keys, expert_ids_turns).reshape((TOKENS, 2))
    route_weights = jnp.clip(0.2 + 0.8 * jax.random.uniform(seeds[3], (TOKENS, 2), jnp.float32) ** block_scale(seeds[3], (TOKENS, 2), ((0, 48),), -0.2, 0.2), 0.2, 1.0)
    w_gate = centred(seeds[4], (EXPERTS, D, FF), D ** -0.5, 0.125, ((0, 48), (2, 16)))
    w_up = centred(seeds[5], (EXPERTS, D, FF), D ** -0.5, 0.125, ((0, 48), (2, 16)))
    w_down = centred(seeds[6], (EXPERTS, FF, D), FF ** -0.5, 0.09375, ((0, 48), (1, 16)))
    return {"tokens": tokens, "norm_gain": norm_gain, "expert_ids": expert_ids, "route_weights": route_weights, "w_gate": w_gate, "w_up": w_up, "w_down": w_down}


epsilon = 1e-06

def run_expert(operands):
    rows, gate_weight, up_weight, down_weight = operands
    model_width = rows.shape[1]
    gate_values = jnp.dot(rows, gate_weight, preferred_element_type=jnp.float32)
    up_values = jnp.dot(rows, up_weight, preferred_element_type=jnp.float32)
    hidden = (jax.nn.silu(gate_values) * up_values).astype(jnp.bfloat16)
    grouped = hidden.reshape(rows.shape[0], N_TP, -1).astype(jnp.float32)
    down_groups = down_weight.reshape(N_TP, -1, model_width).astype(jnp.float32)
    partial_value = jnp.einsum('rtf,tfd->trd', grouped, down_groups)
    partial_value = lax.optimization_barrier(partial_value.astype(jnp.bfloat16)).astype(jnp.float32)
    return lax.optimization_barrier(jnp.sum(partial_value, axis=0)).astype(jnp.bfloat16)

def reference(tokens, norm_gain, expert_ids, route_weights, w_gate, w_up, w_down):
    model_width = tokens.shape[1]
    as_float = tokens.astype(jnp.float32)
    scale = lax.rsqrt(lax.optimization_barrier(jnp.mean(as_float * as_float, axis=-1, keepdims=True)) + epsilon)
    normed = (as_float * scale * norm_gain[None, :]).astype(jnp.bfloat16)
    flat_ids = expert_ids.reshape(N_EP, TOK_DEV * 2).astype(jnp.int32)
    one_hot = (flat_ids[:, :, None] == jnp.arange(EXPERTS, dtype=jnp.int32)[None, None, :]).astype(jnp.int32)
    slot_index = lax.optimization_barrier(jnp.sum((jnp.cumsum(one_hot, axis=1) - one_hot) * one_hot, axis=-1)).astype(jnp.int32)
    source = jnp.arange(N_EP, dtype=jnp.int32)[:, None]
    target = (flat_ids * (N_EP * CAP) + source * CAP + slot_index).reshape(-1).astype(jnp.int32)
    token_rows = jnp.repeat(normed, 2, axis=0)
    buffer = jnp.zeros((EXPERTS * N_EP * CAP, model_width), jnp.bfloat16).at[target].set(token_rows)
    buffer = buffer.reshape(EXPERTS, N_EP * CAP, model_width)
    expert_out = lax.map(run_expert, (buffer, w_gate, w_up, w_down))
    picked = expert_out.reshape(-1, model_width)[target].reshape(TOKENS, 2, model_width).astype(jnp.float32)
    return lax.optimization_barrier(jnp.sum(picked * route_weights[:, :, None], axis=1)).astype(jnp.bfloat16)
```

```python
import functools

import jax
import jax.numpy as jnp
from jax import lax
from jax.experimental import pallas as pl
from jax.experimental.pallas import tpu as pltpu
from jax.sharding import PartitionSpec as P

MESH = pl.DeviceIdType.MESH
EPS = 1e-06
NX = 4
CHUNKS = 3
SKEW = 2


def z_offsets(nz):
    order = [0]
    for d in range(1, nz // 2 + 1):
        order.append(d)
        if d != nz - d:
            order.append(nz - d)
    return order


def kernel(
    sizes,
    tok_ref, gain_ref, ids_ref, rw_ref, wg_hbm, wu_hbm, wd_hbm,
    o_ref,
    wg, wu, wd, outg, X, own, psend, precv, rsend, rrecv, fo, ret, acc,
    w_sem, a2a_send, a2a_recv, gr_send, gr_recv, gp_send, gp_recv,
    rp_send, rp_recv, rr_send, rr_recv, ret_send, ret_recv,
):
    n_ep, ny, cap = sizes
    nz = n_ep // NX
    rows = n_ep * cap
    CR = rows // CHUNKS
    CB = n_ep // CHUNKS
    HP = cap // 2
    CP = CR // 2
    tok = tok_ref.shape[0]
    bf16, f32 = jnp.bfloat16, jnp.float32

    me = lax.axis_index("ep")
    t = lax.axis_index("tp")
    z, x = lax.div(me, NX), lax.rem(me, NX)
    y, c = lax.div(t, 2), lax.rem(t, 2)
    zs = z_offsets(nz)
    offsets = [(dz, dx) for dz in zs for dx in range(NX)]

    def ep_at(sign, p):
        dz, dx = offsets[p]
        return lax.rem(z + (nz + sign * dz) % nz, nz) * NX + lax.rem(x + (NX + sign * dx) % NX, NX)

    right = (me, lax.rem(y + 1, ny) * 2 + c)
    left = (me, lax.rem(y + ny - 1, ny) * 2 + c)
    partner = (me, y * 2 + 1 - c)

    barrier = pltpu.get_barrier_semaphore()
    for p in range(n_ep - 1, 0, -1):
        pl.semaphore_signal(barrier, inc=1, device_id=(ep_at(1, p), t), device_id_type=MESH)
    for peer in (left, right, partner):
        pl.semaphore_signal(barrier, inc=1, device_id=peer, device_id_type=MESH)

    w_copies = [
        pltpu.make_async_copy(src, dst, w_sem.at[i])
        for i, (src, dst) in enumerate(((wg_hbm, wg), (wu_hbm, wu), (wd_hbm, wd)))
    ]
    for copy in w_copies:
        copy.start()

    v = tok_ref[...].astype(f32)
    scale = lax.rsqrt(jnp.mean(v * v, axis=-1, keepdims=True) + EPS)
    mine = pl.ds(pl.multiple_of(t * 128, 128), 128)
    normed = (tok_ref[:, mine].astype(f32) * scale * gain_ref[:, mine]).astype(bf16)

    lanes = lax.broadcasted_iota(jnp.int32, (tok, 128), 1)
    ids = ids_ref[...]
    hit = [ids[:, k : k + 1] == lanes for k in range(2)]
    count = (hit[0] | hit[1]).astype(f32).astype(bf16)
    below = (
        lax.broadcasted_iota(jnp.int32, (tok, tok), 1) < lax.broadcasted_iota(jnp.int32, (tok, tok), 0)
    ).astype(f32).astype(bf16)
    earlier = jnp.dot(below, count, preferred_element_type=f32)
    target = []
    for k in range(2):
        slot = jnp.sum(jnp.where(hit[k], earlier, 0.0), axis=1, keepdims=True).astype(jnp.int32)
        e = ids[:, k : k + 1]
        dz = z - (e >> 2)
        dz = jnp.where(dz < 0, dz + nz, dz)
        dx = x - (e & 3)
        dx = jnp.where(dx < 0, dx + NX, dx)
        rank = jnp.where(dz * 2 <= nz, 2 * dz - 1, 2 * (nz - dz))
        rank = jnp.where(dz == 0, 0, rank)
        target.append((rank * NX + dx) * cap + slot)
    by_lane = [jnp.broadcast_to(a.astype(f32), (tok, tok)).T[0:1, :].astype(jnp.int32) for a in target]
    row = lax.broadcasted_iota(jnp.int32, (rows, tok), 0)
    select = ((row == by_lane[0]) | (row == by_lane[1])).astype(f32).astype(bf16)
    dispatch = jnp.dot(select, normed, preferred_element_type=f32).astype(bf16)
    outg.reshape(rows, 128)[...] = dispatch
    X[0, c, 0:HP] = dispatch[0:cap].reshape(HP, 2, 128)

    pl.semaphore_wait(barrier, n_ep + 2)

    def blocks(ref, p, n=1):
        return ref.at[pl.ds(p * HP, n * HP)]

    def remote(src, dst, ssem, rsem, dev):
        return pltpu.make_async_remote_copy(
            src_ref=src, dst_ref=dst, send_sem=ssem, recv_sem=rsem, device_id=dev, device_id_type=MESH
        )

    pending = []

    def go(*a):
        copy = remote(*a)
        copy.start()
        pending.append(copy)
        return copy

    for p in range(1, n_ep):
        remote(
            blocks(outg, p), blocks(X.at[0, c], p), a2a_send.at[0], a2a_recv.at[p // CB], (ep_at(-1, p), t)
        ).start()

    def pairs(j, lo=0, n=CP):
        return pl.ds(j * CP + lo, n)

    half = CP // 2

    def wait_gather(j, k, lo=0, n=CP, s=None):
        ref = X.at[k, c, pairs(j, lo, n)]
        remote(ref, ref, gr_send.at[j, 0], gr_recv.at[j, k if s is None else s], right).wait_recv()

    def to_partner(j, k):
        ref = X.at[k, c, pairs(j)]
        go(ref, ref, gp_send.at[j, k], gp_recv.at[j, k], partner)

    def forward(j, k, to_right, lo=0, n=CP, s=None):
        k2 = (k - 1) % ny if to_right else (k + 1) % ny
        s = k2 if s is None else s
        go(
            X.at[k, c, pairs(j, lo, n)], X.at[k2, c, pairs(j, lo, n)],
            gr_send.at[j, s], gr_recv.at[j, s], right if to_right else left,
        )

    far = ny // 2

    def gather_step(j, i):
        if i == 0:
            first = 1 if j == 0 else 0
            ref = blocks(X.at[0, c], j * CB + first, CB - first)
            remote(ref, ref, a2a_send.at[0], a2a_recv.at[j], right).wait_recv()
            forward(j, 0, True)
            forward(j, 0, False)
            to_partner(j, 0)
        elif i < far:
            wait_gather(j, ny - i)
            if i < far - 1:
                forward(j, ny - i, True)
            else:
                forward(j, ny - i, True, 0, half, far)
            wait_gather(j, i)
            if i < far - 1:
                forward(j, i, False)
            else:
                forward(j, i, False, half, CP - half, ny)
            to_partner(j, ny - i)
            to_partner(j, i)
        else:
            wait_gather(j, far, 0, half, far)
            wait_gather(j, far, half, CP - half, ny)
            to_partner(j, far)

    order = [far]
    for i in range(far - 1, 0, -1):
        order += [i, ny - i]
    order.append(0)

    def ffn(j):
        if j == 0:
            for copy in w_copies:
                copy.wait()
        gate = up = None
        for k in reversed(order):
            ref = X.at[k, 1 - c, pairs(j)]
            remote(ref, ref, gp_send.at[j, k], gp_recv.at[j, k], partner).wait_recv()
            lhs = jnp.concatenate(
                [X.at[k, q].reshape(rows, 128)[j * CR : (j + 1) * CR, :] for q in range(2)], axis=1
            )
            kk = pl.ds(pl.multiple_of(lax.rem(y + k, ny) * 256, 256), 256)
            dg = jnp.dot(lhs, wg[kk, :], preferred_element_type=f32)
            du = jnp.dot(lhs, wu[kk, :], preferred_element_type=f32)
            gate = dg if gate is None else gate + dg
            up = du if up is None else up + du
        hidden = (gate / (1.0 + jnp.exp(-gate)) * up).astype(bf16)
        for m in order:
            cols = pl.ds(pl.multiple_of(lax.rem(y + m, ny) * 256, 256), 256)
            part = jnp.dot(hidden, wd[:, cols], preferred_element_type=f32)
            lo, hi = part[:, :128], part[:, 128:]
            psend[j, m] = jnp.where(c == 0, hi, lo).astype(bf16)
            own[j, m] = jnp.where(c == 0, lo, hi)
            go(psend.at[j, m], precv.at[j, m], rp_send.at[j, m], rp_recv.at[j, m], partner)

    hr = CR // 2

    def both(j, m, lo, n):
        return own[j, m, lo : lo + n, :] + precv[j, m, lo : lo + n, :].astype(f32)

    def wait_pair(j, m):
        remote(psend.at[j, m], precv.at[j, m], rp_send.at[j, m], rp_recv.at[j, m], partner).wait_recv()

    def ring_wait(j, d, m, lo=0, n=CR):
        ref = rrecv.at[j, d, m, pl.ds(lo, n)]
        remote(ref, ref, rr_send.at[j, d, m], rr_recv.at[j, d, m], right).wait_recv()

    def ring_send(j, d, m, lo=0, n=CR):
        go(
            rsend.at[j, d, m, pl.ds(lo, n)], rrecv.at[j, d, m - 1, pl.ds(lo, n)],
            rr_send.at[j, d, m], rr_recv.at[j, d, m - 1], (right, left)[d],
        )

    def reduce_step(j, i):
        m = far - i
        if i == 0:
            wait_pair(j, far)
            for d, lo in ((0, 0), (1, hr)):
                rsend[j, d, m, lo : lo + hr, :] = both(j, far, lo, hr).astype(bf16)
                ring_send(j, d, m, lo, hr)
        elif i < far:
            for d in range(2):
                mine_m = m if d == 0 else ny - m
                wait_pair(j, mine_m)
                if i == 1:
                    lo = d * hr
                    other = hr - lo
                    rsend[j, d, m, other : other + hr, :] = both(j, mine_m, other, hr).astype(bf16)
                    ring_wait(j, d, m, lo, hr)
                    rsend[j, d, m, lo : lo + hr, :] = (
                        both(j, mine_m, lo, hr) + rrecv[j, d, m, lo : lo + hr, :].astype(f32)
                    ).astype(bf16)
                else:
                    ring_wait(j, d, m)
                    rsend[j, d, m] = (both(j, mine_m, 0, CR) + rrecv[j, d, m].astype(f32)).astype(bf16)
                ring_send(j, d, m)
        else:
            wait_pair(j, 0)
            total = both(j, 0, 0, CR)
            for d in range(2):
                ring_wait(j, d, 0)
                total = total + rrecv[j, d, 0].astype(f32)
            total = total.astype(bf16)
            fo.reshape(rows, 128)[j * CR : (j + 1) * CR, :] = total
            if j == 0:
                ret[0:HP] = total[0:cap].reshape(HP, 2, 128)
            for p in range(max(1, j * CB), (j + 1) * CB):
                remote(
                    blocks(fo, p), blocks(ret, p), ret_send.at[0], ret_recv.at[j], (ep_at(1, p), t)
                ).start()

    def combine(j):
        first = 1 if j == 0 else 0
        ref = blocks(ret, j * CB + first, CB - first)
        remote(ref, ref, ret_send.at[0], ret_recv.at[j], right).wait_recv()
        got = ret.reshape(rows, 128)[j * CR : (j + 1) * CR, :]
        place = lax.broadcasted_iota(jnp.int32, (tok, CR), 1) + j * CR
        total = None
        for k in range(2):
            pick = (place == target[k]).astype(f32).astype(bf16)
            value = jnp.dot(pick, got, preferred_element_type=f32) * rw_ref[:, k : k + 1]
            total = value if total is None else total + value
        if j == 0:
            acc[...] = total
        else:
            acc[...] += total

    stages = [functools.partial(gather_step, i=i) for i in range(far + 1)]
    stages.append(ffn)
    stages += [functools.partial(reduce_step, i=i) for i in range(far + 1)]
    for tick in range(len(stages) + SKEW * (CHUNKS - 1)):
        for j in range(CHUNKS):
            if 0 <= tick - SKEW * j < len(stages):
                stages[tick - SKEW * j](j)
    for j in range(CHUNKS):
        combine(j)
    o_ref[...] = acc[...].astype(bf16)

    ref = blocks(outg, 1, n_ep - 1)
    remote(ref, ref, a2a_send.at[0], a2a_recv.at[0], right).wait_send()
    ref = blocks(fo, 1, n_ep - 1)
    remote(ref, ref, ret_send.at[0], ret_recv.at[0], right).wait_send()
    for copy in pending:
        copy.wait_send()


def per_device(tokens, norm_gain, expert_ids, route_weights, w_gate, w_up, w_down):
    tok, width = tokens.shape
    n_ep, n_tp = lax.axis_size("ep"), lax.axis_size("tp")
    ny = n_tp // 2
    cap = 4 * tok // n_ep
    rows = n_ep * cap
    CR = rows // CHUNKS
    half = ny // 2
    bf16, f32 = jnp.bfloat16, jnp.float32
    vm = pl.BlockSpec(memory_space=pltpu.VMEM)
    hbm = pl.BlockSpec(memory_space=pl.ANY)
    dma = pltpu.SemaphoreType.DMA
    V = pltpu.VMEM
    ff = w_gate.shape[2]
    return pl.pallas_call(
        functools.partial(kernel, (n_ep, ny, cap)),
        out_shape=jax.ShapeDtypeStruct((tok, width // n_tp), bf16),
        in_specs=[vm, vm, vm, vm, hbm, hbm, hbm],
        out_specs=vm,
        scratch_shapes=[
            V((width, ff), bf16), V((width, ff), bf16), V((ff, width), bf16),
            V((rows // 2, 2, 128), bf16),
            V((ny, 2, rows // 2, 2, 128), bf16),
            V((CHUNKS, ny, CR, 128), f32),
            V((CHUNKS, ny, CR, 128), bf16),
            V((CHUNKS, ny, CR, 128), bf16),
            V((CHUNKS, 2, half + 1, CR, 128), bf16),
            V((CHUNKS, 2, half, CR, 128), bf16),
            V((rows // 2, 2, 128), bf16),
            V((rows // 2, 2, 128), bf16),
            V((tok, 128), f32),
            dma((3,)),
            dma((1,)), dma((CHUNKS,)),
            dma((CHUNKS, ny + 1)), dma((CHUNKS, ny + 1)),
            dma((CHUNKS, ny)), dma((CHUNKS, ny)),
            dma((CHUNKS, ny)), dma((CHUNKS, ny)),
            dma((CHUNKS, 2, half + 1)), dma((CHUNKS, 2, half)),
            dma((1,)), dma((CHUNKS,)),
        ],
        compiler_params=pltpu.CompilerParams(
            collective_id=0, has_side_effects=True, vmem_limit_bytes=48 * 1024 * 1024
        ),
        name="experts",
    )(
        tokens, norm_gain.reshape(1, width), expert_ids, route_weights, w_gate[0], w_up[0], w_down[0]
    )


def solution(mesh):
    in_specs = (
        P("ep", None),
        P(),
        P("ep", None),
        P("ep", None),
        P("ep", None, "tp"),
        P("ep", None, "tp"),
        P("ep", "tp", None),
    )
    return jax.shard_map(
        per_device, mesh=mesh, in_specs=in_specs, out_specs=P("ep", "tp"), check_vma=False
    )
```
